32 devices in a mesh: ep: 8 (over z, y), tp: 4 (over x, core).
Axes of the slice: x: 2, y: 2, z: 4, core: 2. Of those that a mesh axis runs over, the one named last changes fastest.
Arguments:
- queries: bfloat16 [4096, 1024], P('ep', 'tp'), may hold values from -6 to 6
- keys: bfloat16 [4096, 512], P('ep', 'tp'), may hold values from -6 to 6
- values: bfloat16 [4096, 512], P('ep', 'tp'), may hold values from -384 to 384
- query_gain: float32 [128], replicated, may hold values from 0.1 to 1.9
- key_gain: float32 [128], replicated, may hold values from 0.1 to 1.9
- out_proj: bfloat16 [1024, 2048], replicated, may hold values from -0.1875 to 0.1875
- tokens_b: bfloat16 [4096, 2048], P(('ep', 'tp')), may hold values from -6 to 6
- norm_gain: float32 [2048], replicated, may hold values from 0.1 to 1.9
- routes: int32 [4096, 2], P(('ep', 'tp')), may hold values from 0 to 31, all different within a row; in each aligned block of 128 rows (0 to 127, 128 to 255, ...) at most 16 rows name the same one
- group_prob: float32 [4096], P(('ep', 'tp')), may hold values from 0.25 to 1
- expert_logits: float32 [4096, 2], P(('ep', 'tp')), may hold values from -6 to 6
- w_gate: bfloat16 [32, 2048, 512], P(('ep', 'tp')), may hold values from -0.125 to 0.125
- w_up: bfloat16 [32, 2048, 512], P(('ep', 'tp')), may hold values from -0.125 to 0.125
- w_down: bfloat16 [32, 512, 2048], P(('ep', 'tp')), may hold values from -0.25 to 0.25
Outputs:
- mixed_a: bfloat16 [4096, 2048], P(('ep', 'tp'))
- mixed_b: bfloat16 [4096, 2048], P(('ep', 'tp'))
The draws below stay inside these ranges and needn't reach their ends.
Inputs may be any that keep to these rules, and one draw needn't show every extreme that they name: Within the 128 rows of one device, no expert is named by more than 16 of the routes, and in every draw some expert is named exactly 16 times by the rows of some device. The 2 experts of a row differ.
All inputs are finite; a program needn't handle non-finite values.
Results may differ from the reference program's by a relative error of at most 0.014.
Values may be sent and summed in bfloat16 or wider, within the bound.
A program may use at most 128 MiB of HBM per device.

```python
import math
import jax
import jax.numpy as jnp
import numpy as np
from jax import lax

D = 2048
HEADS = 8
KV_HEADS = 4
HD = 128
FF_E = 512
GRID_W = 64
TOP_K = 2
TOK_B = 128
SEQ = 4096
TOKENS_B = 4096
EXPERTS = 32
CAP = 16
N_EP = 8
N_TP = 4


def levels(own_key, dims, split, low, high):
    level, own = 1.0, jax.random.fold_in(own_key, 6)
    for axis_at, blocks in split:
        heights = jnp.exp(jax.random.uniform(jax.random.fold_in(own, axis_at), (blocks,), jnp.float32, low / len(split), high / len(split)))
        level = level * jnp.repeat(heights, dims[axis_at] // blocks).reshape([-1 if axis == axis_at else 1 for axis in range(len(dims))])
    return level


def assign_block(key, own, number, rows, number_of, top, bound, lean):
    sequence = jax.random.permutation(key, number_of)
    packed, common = portions_of(number_of, rows * top, bound, lean, True), portions_of(number_of, rows * top, bound, lean, False)
    places = jnp.arange(number_of)

    def named(sizes, turn):
        used = int((sizes > 0).sum())
        fixed = max(1, used // 4)
        moved = fixed + (places - fixed + turn * (used - fixed)) % max(1, number_of - fixed)
        return jnp.zeros((number_of,), jnp.int32).at[sequence[jnp.where(places < fixed, places, moved)]].set(jnp.asarray(sizes, jnp.int32))

    sizes = jnp.where(number % 4 == 0, named(packed, number // 4), named(common, number - number // 4 - 1))
    mixed = jax.random.permutation(jax.random.fold_in(own, 3), number_of)
    source_of, receiver = mixed[0:number_of // 2 * 2:2], mixed[1:number_of // 2 * 2:2]
    slack = jnp.minimum(sizes[source_of] - 1, bound - sizes[receiver]) // 2
    slack = jnp.where((source_of == sequence[0]) | (receiver == sequence[0]) | (sizes[receiver] == 0), 0, jnp.maximum(slack, 0))
    moved = jax.random.randint(jax.random.fold_in(own, 4), (number_of // 2,), 0, 1 << 20) % (slack + 1)
    sizes = sizes.at[source_of].add(-moved).at[receiver].add(moved)
    members = jnp.searchsorted(jnp.cumsum(sizes), jnp.arange(rows * top), side="right").astype(jnp.int32)
    table = members.reshape(top, rows).T
    table = table[jax.random.permutation(jax.random.fold_in(own, 1), rows)]
    turn = jax.random.randint(jax.random.fold_in(own, 2), (rows, 1), 0, top)
    return jnp.take_along_axis(table, (jnp.arange(top)[None, :] + turn) % top, axis=1)


def portions_of(number_of, total, limit, skew, full):
    portions = [(1 << 20) // math.isqrt(standing ** skew) + 1 for standing in range(1, number_of + 1)]
    largest = limit if full else min(limit, max(-(-total // number_of), total * portions[0] // sum(portions)))
    least = 1 if total - largest >= number_of - 1 else 0
    given, spare = [largest] + [least] * (number_of - 1), total - largest - least * (number_of - 1)
    while spare > 0:
        movable = [i for i in range(1, number_of) if given[i] < largest] or [i for i in range(1, number_of) if given[i] < limit]
        pool, left = sum([portions[i] for i in movable]), spare
        for i in movable:
            more = min(limit - given[i], max(1, left * portions[i] // pool), spare)
            given[i] = given[i] + more
            spare = spare - more
    return np.array(given)


def bell_draw(own_key, dims, scale, most, pieces=(), kind=jnp.bfloat16):
    loudness = levels(own_key, dims, pieces, -0.22, 0.18) if pieces else 1.0
    array = jax.random.normal(own_key, dims, jnp.float32) * scale * loudness
    return jnp.minimum(jnp.maximum(array, -most), most).astype(kind)


def setup_inputs(seed: int = 0) -> dict:
    splits = jax.random.split(jax.random.key(seed), 15)
    queries = bell_draw(splits[0], (SEQ, HEADS * HD), 1.0, 6.0, ((0, 8), (1, 4)))
    keys = bell_draw(splits[1], (SEQ, KV_HEADS * HD), 1.0, 6.0, ((0, 8), (1, 4)))
    values = bell_draw(splits[2], (SEQ, KV_HEADS * HD), 64.0, 384.0, ((0, 8), (1, 4)))
    query_gain = jnp.clip(1.0 + 0.18 * jax.random.normal(splits[3], (HD,), jnp.float32), 0.1, 1.9)
    key_gain = jnp.clip(1.0 + 0.18 * jax.random.normal(splits[4], (HD,), jnp.float32), 0.1, 1.9)
    out_proj = bell_draw(splits[5], (HEADS * HD, D), (HEADS * HD) ** -0.5, 0.1875)
    tokens_b = bell_draw(splits[6], (TOKENS_B, D), 1.0, 6.0, ((0, 32),))
    norm_gain = jnp.clip(1.0 + 0.18 * jax.random.normal(splits[7], (D,), jnp.float32), 0.1, 1.9)
    routes_keys = jax.random.split(jax.random.fold_in(splits[8], 1), TOKENS_B // TOK_B)
    routes_turns = jax.random.permutation(jax.random.fold_in(splits[8], 3), TOKENS_B // TOK_B)
    routes = jax.vmap(lambda own, number: assign_block(jax.random.fold_in(splits[8], 2), own, number, TOK_B, EXPERTS, TOP_K, CAP, 1))(routes_keys, routes_turns).reshape((TOKENS_B, TOP_K))
    group_prob = jnp.clip(0.25 + 0.75 * jax.random.uniform(splits[9], (TOKENS_B,), jnp.float32) ** levels(splits[9], (TOKENS_B,), ((0, 32),), -0.2, 0.2), 0.25, 1.0)
    expert_logits = bell_draw(splits[10], (TOKENS_B, TOP_K), 1.5, 6.0, ((0, 32),), jnp.float32)
    w_gate = bell_draw(splits[11], (EXPERTS, D, FF_E), D ** -0.5, 0.125, ((0, 32),))
    w_up = bell_draw(splits[12], (EXPERTS, D, FF_E), D ** -0.5, 0.125, ((0, 32),))
    w_down = bell_draw(splits[13], (EXPERTS, FF_E, D), FF_E ** -0.5, 0.25, ((0, 32),))
    return {"queries": queries, "keys": keys, "values": values, "query_gain": query_gain, "key_gain": key_gain, "out_proj": out_proj, "tokens_b": tokens_b, "norm_gain": norm_gain, "routes": routes, "group_prob": group_prob, "expert_logits": expert_logits, "w_gate": w_gate, "w_up": w_up, "w_down": w_down}


NORM_EPS = 1e-06
ROPE_BASE = 10000.0

def rope_angles(row_count, offset, head_dim):
    quarter = head_dim // 4
    position = offset + jnp.arange(row_count, dtype=jnp.int32)
    grid_row = (position // GRID_W).astype(jnp.float32)
    grid_col = (position % GRID_W).astype(jnp.float32)
    frequency = ROPE_BASE ** (-jnp.arange(quarter, dtype=jnp.float32) / quarter)
    angles = jnp.concatenate([grid_row[:, None] * frequency, grid_col[:, None] * frequency], axis=1)
    return (jnp.cos(angles), jnp.sin(angles))

def norm_rotate(block_in, gain, cos_table, sin_table):
    wide = block_in.astype(jnp.float32)
    wide = wide * lax.rsqrt(lax.optimization_barrier(jnp.mean(wide * wide, axis=-1, keepdims=True)) + NORM_EPS) * gain
    half_width = wide.shape[-1] // 2
    first_half, second_half = (wide[..., :half_width], wide[..., half_width:])
    cos_b = cos_table[:, None, :]
    sin_b = sin_table[:, None, :]
    turned = jnp.concatenate([first_half * cos_b - second_half * sin_b, second_half * cos_b + first_half * sin_b], axis=-1)
    return turned.astype(jnp.bfloat16)

def reference(queries, keys, values, query_gain, key_gain, out_proj, tokens_b, norm_gain, routes, group_prob, expert_logits, w_gate, w_up, w_down):
    group_size = HEADS // KV_HEADS
    cos_table, sin_table = rope_angles(SEQ, 0, HD)
    qrot = norm_rotate(queries.reshape(SEQ, HEADS, HD), query_gain, cos_table, sin_table)
    qrot = qrot.reshape(SEQ, KV_HEADS, group_size, HD)
    krot = norm_rotate(keys.reshape(SEQ, KV_HEADS, HD), key_gain, cos_table, sin_table).astype(jnp.float32)
    value_heads = values.reshape(SEQ, KV_HEADS, HD).astype(jnp.float32)
    query_block = math.gcd(SEQ, 256)

    def one_block(row_start):
        chosen = lax.dynamic_slice_in_dim(qrot, row_start, query_block, 0).astype(jnp.float32)
        scores = jnp.einsum('qhgd,khd->qhgk', chosen, krot) * HD ** (-0.5)
        weights = jnp.exp(scores).astype(jnp.bfloat16).astype(jnp.float32)
        denominator = lax.optimization_barrier(jnp.sum(weights, axis=-1))
        numerator = jnp.einsum('qhgk,khd->qhgd', weights, value_heads)
        return (numerator / denominator[..., None]).astype(jnp.bfloat16)
    starts = (jnp.arange(SEQ // query_block, dtype=jnp.int32) * query_block).astype(jnp.int32)
    attended = lax.map(one_block, starts).reshape(SEQ, HEADS * HD)
    mixed_a = jnp.dot(attended, out_proj, preferred_element_type=jnp.float32).astype(jnp.bfloat16)
    wide_b = tokens_b.astype(jnp.float32)
    normed = (wide_b * lax.rsqrt(lax.optimization_barrier(jnp.mean(wide_b * wide_b, axis=-1, keepdims=True)) + NORM_EPS) * norm_gain).astype(jnp.bfloat16)
    combine = group_prob[:, None] * jax.nn.softmax(expert_logits, axis=-1)
    combine_flat = combine.reshape(-1)
    device_count = N_EP * N_TP
    per_device = TOK_B * TOP_K
    flat_routes = routes.reshape(device_count, per_device)
    onehot = (flat_routes[:, :, None] == jnp.arange(EXPERTS, dtype=jnp.int32)[None, None, :]).astype(jnp.int32)
    slot_rank = lax.optimization_barrier(jnp.sum((jnp.cumsum(onehot, axis=1) - onehot) * onehot, axis=2)).astype(jnp.int32)
    source = jnp.broadcast_to(jnp.arange(device_count, dtype=jnp.int32)[:, None], (device_count, per_device))
    assign_ids = (source * per_device + jnp.arange(per_device, dtype=jnp.int32)[None, :]).astype(jnp.int32)
    slot_table = jnp.zeros((EXPERTS, device_count, CAP), jnp.int32).at[flat_routes, source, slot_rank].set(assign_ids + 1)
    slot_table = slot_table.reshape(EXPERTS, device_count * CAP)

    def per_expert(accumulated, expert_args):
        slot_ids, gate_w, up_w, down_w = expert_args
        live_slots = slot_ids > 0
        assign = jnp.maximum(slot_ids - 1, 0).astype(jnp.int32)
        token_index = (assign // TOP_K).astype(jnp.int32)
        inputs = jnp.where(live_slots[:, None], normed[token_index], jnp.zeros((), jnp.bfloat16))
        gate_part = jnp.dot(inputs, gate_w, preferred_element_type=jnp.float32)
        up_part = jnp.dot(inputs, up_w, preferred_element_type=jnp.float32)
        hidden = (jax.nn.silu(gate_part) * up_part).astype(jnp.bfloat16)
        expert_out = jnp.dot(hidden, down_w, preferred_element_type=jnp.float32).astype(jnp.bfloat16)
        factor = jnp.where(live_slots, combine_flat[assign], jnp.zeros((), jnp.float32))
        return (accumulated.at[token_index].add(factor[:, None] * expert_out.astype(jnp.float32)), None)
    accumulated = lax.scan(per_expert, jnp.zeros((TOKENS_B, D), jnp.float32), (slot_table, w_gate, w_up, w_down))[0]
    mixed_b = accumulated.astype(jnp.bfloat16)
    return (mixed_a, mixed_b)
```

```python
import functools
import math

import jax
import jax.numpy as jnp
from jax import lax
from jax.experimental import pallas as pl
from jax.experimental.pallas import tpu as pltpu
from jax.sharding import PartitionSpec as P

GRID_W = 64


NORM_EPS = 1e-06
ROPE_BASE = 10000.0
VMEM = pl.BlockSpec(memory_space=pltpu.VMEM)


def rope_angles(row_count, offset, head_dim):
    quarter = head_dim // 4
    position = offset + jnp.arange(row_count, dtype=jnp.int32)
    grid_row = (position // GRID_W).astype(jnp.float32)
    grid_col = (position % GRID_W).astype(jnp.float32)
    frequency = ROPE_BASE ** (-jnp.arange(quarter, dtype=jnp.float32) / quarter)
    angles = jnp.concatenate([grid_row[:, None] * frequency, grid_col[:, None] * frequency], axis=1)
    return (jnp.cos(angles), jnp.sin(angles))


def norm_rotate(wide, gain, cos_table, sin_table):
    wide = wide * lax.rsqrt(jnp.mean(wide * wide, axis=-1, keepdims=True) + NORM_EPS) * gain
    half_width = wide.shape[-1] // 2
    first_half, second_half = (wide[..., :half_width], wide[..., half_width:])
    return jnp.concatenate(
        [
            first_half * cos_table - second_half * sin_table,
            second_half * cos_table + first_half * sin_table,
        ],
        axis=-1,
    )


def gather_pieces(block):
    count = lax.axis_size("ep")
    rows = block.shape[0]
    if count % 2 or count < 4:
        return [lax.all_gather(block, "ep", axis=0, tiled=True)]
    partner = lax.ppermute(block, "ep", [(i, i ^ 1) for i in range(count)])
    block = jnp.concatenate([block, partner], axis=0)
    outer = count // 2
    ahead = [(i, (i // 2 + 1) % outer * 2 + i % 2) for i in range(count)]
    behind = [(i, (i // 2 - 1) % outer * 2 + i % 2) for i in range(count)]
    pieces = [block]
    right, left = block, block
    for _ in range((outer - 1) // 2):
        right = lax.ppermute(right, "ep", ahead)
        left = lax.ppermute(left, "ep", behind)
        pieces += [right, left]
    if outer % 2 == 0:
        pieces.append(lax.ppermute(right[:rows], "ep", ahead))
        pieces.append(lax.ppermute(left[rows:], "ep", behind))
    return pieces


def attention_kernel(piece_count, head_dim, chunk, q_ref, *refs):
    pieces = refs[:piece_count]
    out_ref, wide_values = refs[piece_count], refs[piece_count + 1]
    queries = q_ref[...]
    total = jnp.zeros((queries.shape[0], 2 * head_dim), jnp.float32)
    base = 0
    first = (pl.program_id(0) == 0) & (pl.program_id(1) == 0)

    @pl.when(first)
    def _():
        at = 0
        for piece in pieces:
            rows = piece.shape[0]
            wide_values[at : at + rows, :head_dim] = piece[:, head_dim:]
            wide_values[at : at + rows, head_dim:] = jnp.ones((rows, head_dim), jnp.bfloat16)
            at += rows

    for piece in pieces:
        rows = piece.shape[0]
        step = math.gcd(rows, chunk)
        for start in range(0, rows, step):
            scores = lax.dot_general(
                queries,
                piece[start : start + step, :head_dim],
                (((1,), (1,)), ((), ())),
                preferred_element_type=jnp.float32,
            )
            weights = jnp.exp2(scores).astype(jnp.bfloat16)
            total = total + jnp.dot(
                weights,
                wide_values[base + start : base + start + step, :],
                preferred_element_type=jnp.float32,
            )
        base += rows
    out_ref[...] = (total[:, :head_dim] / total[:, head_dim:]).astype(jnp.bfloat16)


def attend(queries, pieces, head_dim):
    row_count, width = queries.shape
    heads = width // head_dim
    tile = math.gcd(row_count, 256)
    key_count = sum(piece.shape[0] for piece in pieces)
    spec = pl.BlockSpec((tile, head_dim), lambda h, r: (r, h))
    return pl.pallas_call(
        functools.partial(attention_kernel, len(pieces), head_dim, 512),
        out_shape=jax.ShapeDtypeStruct((row_count, width), jnp.bfloat16),
        grid=(heads, row_count // tile),
        in_specs=[spec] + [VMEM] * len(pieces),
        out_specs=spec,
        scratch_shapes=[pltpu.VMEM((key_count, 2 * head_dim), jnp.bfloat16)],
        cost_estimate=pl.CostEstimate(
            flops=8 * row_count * width * key_count,
            bytes_accessed=4 * row_count * width + 4 * key_count * head_dim,
            transcendentals=heads * row_count * key_count,
        ),
        name="attend",
    )(queries, *pieces)


def attention_inputs(queries, keys, values, query_gain, key_gain):
    row_count = queries.shape[0]
    head_dim = query_gain.shape[0]
    heads = queries.shape[1] // head_dim
    assert keys.shape[1] == head_dim
    cos_table, sin_table = rope_angles(row_count, lax.axis_index("ep") * row_count, head_dim)
    krot = norm_rotate(keys.astype(jnp.float32), key_gain, cos_table, sin_table)
    block = jnp.concatenate([krot.astype(jnp.bfloat16), values], axis=1)
    factor = head_dim ** (-0.5) * math.log2(math.e)
    wide = queries.astype(jnp.float32)
    turned = [
        norm_rotate(wide[:, h * head_dim : (h + 1) * head_dim], query_gain, cos_table, sin_table)
        for h in range(heads)
    ]
    return (jnp.concatenate(turned, axis=1) * factor).astype(jnp.bfloat16), block


def project(attended, out_proj):
    tp_count = lax.axis_size("tp")
    row_count, width = attended.shape
    part = row_count // tp_count
    arrived = lax.all_to_all(
        attended.reshape(tp_count, part, width), "tp", split_axis=0, concat_axis=0, tiled=True
    )
    own = arrived.transpose(1, 0, 2).reshape(part, tp_count * width)
    return jnp.dot(own, out_proj, preferred_element_type=jnp.float32).astype(jnp.bfloat16)


def slot_matrix(slot_row, slot_count):
    row_count = slot_row.shape[1]
    places = lax.broadcasted_iota(jnp.int32, (slot_count, row_count), 0)
    return jnp.where(places == slot_row, 1.0, 0.0).astype(jnp.bfloat16)


def dispatch_kernel(capacity, experts, routes_ref, tokens_ref, gain_ref, sender_ref, slots_ref):
    top_count, row_count = routes_ref.shape
    wide = tokens_ref[...].astype(jnp.float32)
    normed = wide * lax.rsqrt(jnp.mean(wide * wide, axis=-1, keepdims=True) + NORM_EPS)
    normed = (normed * gain_ref[...]).astype(jnp.bfloat16)
    before = lax.broadcasted_iota(jnp.int32, (row_count, row_count), 0)
    before = before < lax.broadcasted_iota(jnp.int32, (row_count, row_count), 1)
    before = jnp.where(before, 1.0, 0.0).astype(jnp.bfloat16)
    names = lax.broadcasted_iota(jnp.int32, (experts, row_count), 0)
    taken = jnp.zeros((experts, 1), jnp.float32)
    chosen = None
    for k in range(top_count):
        route = routes_ref[k : k + 1, :]
        onehot = jnp.where(names == route, 1.0, 0.0)
        ahead = jnp.dot(
            onehot.astype(jnp.bfloat16), before, preferred_element_type=jnp.float32
        )
        rank = jnp.sum((ahead + taken) * onehot, axis=0, keepdims=True)
        taken = taken + jnp.sum(onehot, axis=1, keepdims=True)
        slot = route * capacity + rank.astype(jnp.int32)
        slots_ref[k : k + 1, :] = slot
        part = slot_matrix(slot, experts * capacity)
        chosen = part if chosen is None else chosen + part
    sender_ref[...] = jnp.dot(chosen, normed, preferred_element_type=jnp.float32).astype(
        jnp.bfloat16
    )


def combine_kernel(slots_ref, prob_ref, logits_ref, returned_ref, out_ref):
    top_count = slots_ref.shape[0]
    slot_count = returned_ref.shape[0]
    logits = logits_ref[...]
    raised = jnp.exp(logits - jnp.max(logits, axis=1, keepdims=True))
    share = prob_ref[...] * (raised / jnp.sum(raised, axis=1, keepdims=True))
    total = None
    for k in range(top_count):
        picked = lax.dot_general(
            slot_matrix(slots_ref[k : k + 1, :], slot_count),
            returned_ref[...],
            (((0,), (0,)), ((), ())),
            preferred_element_type=jnp.float32,
        )
        term = picked * share[:, k : k + 1]
        total = term if total is None else total + term
    out_ref[...] = total.astype(jnp.bfloat16)


def expert_kernel(x_ref, gate_ref, up_ref, down_ref, out_ref, total):
    inputs = x_ref[...]
    gate_part = jnp.dot(inputs, gate_ref[...], preferred_element_type=jnp.float32)
    up_part = jnp.dot(inputs, up_ref[...], preferred_element_type=jnp.float32)
    hidden = (gate_part / (1.0 + jnp.exp(-gate_part)) * up_part).astype(jnp.bfloat16)
    part = jnp.dot(hidden, down_ref[...], preferred_element_type=jnp.float32)

    @pl.when(pl.program_id(0) == 0)
    def _():
        total[...] = part

    @pl.when(pl.program_id(0) != 0)
    def _():
        total[...] += part

    @pl.when(pl.program_id(0) == pl.num_programs(0) - 1)
    def _():
        out_ref[...] = total[...].astype(jnp.bfloat16)


def expert_apply(inputs, gate_w, up_w, down_w):
    rows, width = inputs.shape
    hidden = gate_w.shape[1]
    tile = math.gcd(hidden, 256)
    return pl.pallas_call(
        expert_kernel,
        out_shape=jax.ShapeDtypeStruct((rows, width), jnp.bfloat16),
        grid=(hidden // tile,),
        in_specs=[
            VMEM,
            pl.BlockSpec((width, tile), lambda i: (0, i)),
            pl.BlockSpec((width, tile), lambda i: (0, i)),
            pl.BlockSpec((tile, width), lambda i: (i, 0)),
        ],
        out_specs=VMEM,
        scratch_shapes=[pltpu.VMEM((rows, width), jnp.float32)],
        cost_estimate=pl.CostEstimate(
            flops=6 * rows * width * hidden,
            bytes_accessed=6 * width * hidden + 4 * rows * width,
            transcendentals=rows * hidden,
        ),
        name="experts",
    )(inputs, gate_w, up_w, down_w)


def body(
    queries,
    keys,
    values,
    query_gain,
    key_gain,
    out_proj,
    tokens_b,
    norm_gain,
    routes,
    group_prob,
    expert_logits,
    w_gate,
    w_up,
    w_down,
):
    device_count = lax.axis_size("ep") * lax.axis_size("tp")
    row_count, top_count = routes.shape
    model_width = tokens_b.shape[1]
    capacity = 2 * top_count * row_count // device_count
    head_dim = query_gain.shape[0]

    queries_in, block = attention_inputs(queries, keys, values, query_gain, key_gain)
    sender, slots = pl.pallas_call(
        functools.partial(dispatch_kernel, capacity, device_count),
        out_shape=(
            jax.ShapeDtypeStruct((device_count * capacity, model_width), jnp.bfloat16),
            jax.ShapeDtypeStruct((top_count, row_count), jnp.int32),
        ),
        in_specs=[VMEM] * 3,
        out_specs=(VMEM, VMEM),
        name="dispatch",
    )(routes.T, tokens_b, norm_gain.reshape(1, model_width))

    def exchange(rows):
        return lax.all_to_all(
            rows.reshape(device_count, capacity, model_width),
            ("ep", "tp"),
            split_axis=0,
            concat_axis=0,
            tiled=True,
        ).reshape(device_count * capacity, model_width)

    pieces = gather_pieces(block)
    arrived = exchange(sender)
    expert_out = expert_apply(arrived, w_gate[0], w_up[0], w_down[0])
    returned = exchange(expert_out)
    attended = attend(queries_in, pieces, head_dim)
    mixed_a = project(attended, out_proj)
    mixed_b = pl.pallas_call(
        combine_kernel,
        out_shape=jax.ShapeDtypeStruct((row_count, model_width), jnp.bfloat16),
        in_specs=[VMEM] * 4,
        out_specs=VMEM,
        name="combine",
    )(slots, group_prob.reshape(row_count, 1), expert_logits, returned)
    return (mixed_a, mixed_b)


def solution(mesh):
    placed = (
        P("ep", "tp"),
        P("ep", "tp"),
        P("ep", "tp"),
        P(),
        P(),
        P(),
        P(("ep", "tp"), None),
        P(),
        P(("ep", "tp"), None),
        P(("ep", "tp")),
        P(("ep", "tp"), None),
        P(("ep", "tp"), None, None),
        P(("ep", "tp"), None, None),
        P(("ep", "tp"), None, None),
    )
    return jax.shard_map(
        body,
        mesh=mesh,
        in_specs=placed,
        out_specs=(P(("ep", "tp"), None), P(("ep", "tp"), None)),
        check_vma=False,
    )
```

```python
import functools
import math

import jax
import jax.numpy as jnp
from jax import lax
from jax.experimental import pallas as pl
from jax.experimental.pallas import tpu as pltpu
from jax.sharding import PartitionSpec as P

GRID_W = 64


NORM_EPS = 1e-06
ROPE_BASE = 10000.0
VMEM = pl.BlockSpec(memory_space=pltpu.VMEM)


def rope_angles(row_count, offset, head_dim):
    quarter = head_dim // 4
    position = offset + jnp.arange(row_count, dtype=jnp.int32)
    grid_row = (position // GRID_W).astype(jnp.float32)
    grid_col = (position % GRID_W).astype(jnp.float32)
    frequency = ROPE_BASE ** (-jnp.arange(quarter, dtype=jnp.float32) / quarter)
    angles = jnp.concatenate([grid_row[:, None] * frequency, grid_col[:, None] * frequency], axis=1)
    return (jnp.cos(angles), jnp.sin(angles))


def norm_rotate(wide, gain, cos_table, sin_table):
    wide = wide * lax.rsqrt(jnp.mean(wide * wide, axis=-1, keepdims=True) + NORM_EPS) * gain
    half_width = wide.shape[-1] // 2
    first_half, second_half = (wide[..., :half_width], wide[..., half_width:])
    return jnp.concatenate(
        [
            first_half * cos_table - second_half * sin_table,
            second_half * cos_table + first_half * sin_table,
        ],
        axis=-1,
    )


def gather_pieces(block, gate):
    count = lax.axis_size("ep")
    rows = block.shape[0]
    if count % 2 or count < 4:
        return [lax.all_gather(block, "ep", axis=0, tiled=True)], gate
    outer = count // 2
    swap = [(i, i ^ 1) for i in range(count)]
    if outer <= 4:
        ahead = [(i, i + 2) for i in range(count - 2)]
        behind = [(i + 2, i) for i in range(count - 2)]
        rights, lefts = [block], [block]
        pieces = [block, lax.ppermute(block, "ep", swap)]
        for step in range(1, outer):
            rights.append(lax.ppermute(rights[-1], "ep", ahead))
            lefts.append(lax.ppermute(lefts[-1], "ep", behind))
            if step == 1:
                gate, rights[1], lefts[1], pieces[1] = lax.optimization_barrier(
                    (gate, rights[1], lefts[1], pieces[1])
                )
        for step in range(1, outer):
            piece = rights[step] + lefts[outer - step]
            pieces += [piece, lax.ppermute(piece, "ep", swap)]
        return pieces, gate
    partner = lax.ppermute(block, "ep", swap)
    block = jnp.concatenate([block, partner], axis=0)
    ahead = [(i, (i // 2 + 1) % outer * 2 + i % 2) for i in range(count)]
    behind = [(i, (i // 2 - 1) % outer * 2 + i % 2) for i in range(count)]
    pieces = [block]
    right, left = block, block
    for _ in range((outer - 1) // 2):
        right = lax.ppermute(right, "ep", ahead)
        left = lax.ppermute(left, "ep", behind)
        pieces += [right, left]
    if outer % 2 == 0:
        pieces.append(lax.ppermute(right[:rows], "ep", ahead))
        pieces.append(lax.ppermute(left[rows:], "ep", behind))
    return pieces, gate


def attention_kernel(piece_count, head_dim, chunk, q_ref, *refs):
    pieces = refs[:piece_count]
    out_ref, wide_values = refs[piece_count], refs[piece_count + 1]
    queries = q_ref[...]
    total = jnp.zeros((queries.shape[0], 2 * head_dim), jnp.float32)
    base = 0
    first = (pl.program_id(0) == 0) & (pl.program_id(1) == 0)

    @pl.when(first)
    def _():
        at = 0
        for piece in pieces:
            rows = piece.shape[0]
            wide_values[at : at + rows, :head_dim] = piece[:, head_dim:]
            wide_values[at : at + rows, head_dim:] = jnp.ones((rows, head_dim), jnp.bfloat16)
            at += rows

    for piece in pieces:
        rows = piece.shape[0]
        step = math.gcd(rows, chunk)
        for start in range(0, rows, step):
            scores = lax.dot_general(
                queries,
                piece[start : start + step, :head_dim],
                (((1,), (1,)), ((), ())),
                preferred_element_type=jnp.float32,
            )
            weights = jnp.exp2(scores).astype(jnp.bfloat16)
            total = total + jnp.dot(
                weights,
                wide_values[base + start : base + start + step, :],
                preferred_element_type=jnp.float32,
            )
        base += rows
    out_ref[...] = (total[:, :head_dim] / total[:, head_dim:]).astype(jnp.bfloat16)


def attend(queries, pieces, head_dim):
    row_count, width = queries.shape
    heads = width // head_dim
    tile = math.gcd(row_count, 256)
    key_count = sum(piece.shape[0] for piece in pieces)
    spec = pl.BlockSpec((tile, head_dim), lambda h, r: (r, h))
    return pl.pallas_call(
        functools.partial(attention_kernel, len(pieces), head_dim, 512),
        out_shape=jax.ShapeDtypeStruct((row_count, width), jnp.bfloat16),
        grid=(heads, row_count // tile),
        in_specs=[spec] + [VMEM] * len(pieces),
        out_specs=spec,
        scratch_shapes=[pltpu.VMEM((key_count, 2 * head_dim), jnp.bfloat16)],
        cost_estimate=pl.CostEstimate(
            flops=8 * row_count * width * key_count,
            bytes_accessed=4 * row_count * width + 4 * key_count * head_dim,
            transcendentals=heads * row_count * key_count,
        ),
        name="attend",
    )(queries, *pieces)


def attention_inputs(queries, keys, values, query_gain, key_gain):
    row_count = queries.shape[0]
    head_dim = query_gain.shape[0]
    heads = queries.shape[1] // head_dim
    assert keys.shape[1] == head_dim
    cos_table, sin_table = rope_angles(row_count, lax.axis_index("ep") * row_count, head_dim)
    krot = norm_rotate(keys.astype(jnp.float32), key_gain, cos_table, sin_table)
    block = jnp.concatenate([krot.astype(jnp.bfloat16), values], axis=1)
    factor = head_dim ** (-0.5) * math.log2(math.e)
    wide = queries.astype(jnp.float32)
    turned = [
        norm_rotate(wide[:, h * head_dim : (h + 1) * head_dim], query_gain, cos_table, sin_table)
        for h in range(heads)
    ]
    return (jnp.concatenate(turned, axis=1) * factor).astype(jnp.bfloat16), block


def project(attended, out_proj):
    tp_count = lax.axis_size("tp")
    row_count, width = attended.shape
    part = row_count // tp_count
    arrived = lax.all_to_all(
        attended.reshape(tp_count, part, width), "tp", split_axis=0, concat_axis=0, tiled=True
    )
    own = arrived.transpose(1, 0, 2).reshape(part, tp_count * width)
    return jnp.dot(own, out_proj, preferred_element_type=jnp.float32).astype(jnp.bfloat16)


def slot_matrix(slot_row, slot_count):
    row_count = slot_row.shape[1]
    places = lax.broadcasted_iota(jnp.int32, (slot_count, row_count), 0)
    return jnp.where(places == slot_row, 1.0, 0.0).astype(jnp.bfloat16)


def dispatch_kernel(capacity, experts, routes_ref, tokens_ref, gain_ref, sender_ref, slots_ref):
    top_count, row_count = routes_ref.shape
    wide = tokens_ref[...].astype(jnp.float32)
    normed = wide * lax.rsqrt(jnp.mean(wide * wide, axis=-1, keepdims=True) + NORM_EPS)
    normed = (normed * gain_ref[...]).astype(jnp.bfloat16)
    before = lax.broadcasted_iota(jnp.int32, (row_count, row_count), 0)
    before = before < lax.broadcasted_iota(jnp.int32, (row_count, row_count), 1)
    before = jnp.where(before, 1.0, 0.0).astype(jnp.bfloat16)
    names = lax.broadcasted_iota(jnp.int32, (experts, row_count), 0)
    taken = jnp.zeros((experts, 1), jnp.float32)
    chosen = None
    for k in range(top_count):
        route = routes_ref[k : k + 1, :]
        onehot = jnp.where(names == route, 1.0, 0.0)
        ahead = jnp.dot(
            onehot.astype(jnp.bfloat16), before, preferred_element_type=jnp.float32
        )
        rank = jnp.sum((ahead + taken) * onehot, axis=0, keepdims=True)
        taken = taken + jnp.sum(onehot, axis=1, keepdims=True)
        slot = route * capacity + rank.astype(jnp.int32)
        slots_ref[k : k + 1, :] = slot
        part = slot_matrix(slot, experts * capacity)
        chosen = part if chosen is None else chosen + part
    sender_ref[...] = jnp.dot(chosen, normed, preferred_element_type=jnp.float32).astype(
        jnp.bfloat16
    )


def combine_kernel(slots_ref, prob_ref, logits_ref, returned_ref, out_ref):
    top_count = slots_ref.shape[0]
    slot_count = returned_ref.shape[0]
    logits = logits_ref[...]
    raised = jnp.exp(logits - jnp.max(logits, axis=1, keepdims=True))
    share = prob_ref[...] * (raised / jnp.sum(raised, axis=1, keepdims=True))
    total = None
    for k in range(top_count):
        picked = lax.dot_general(
            slot_matrix(slots_ref[k : k + 1, :], slot_count),
            returned_ref[...],
            (((0,), (0,)), ((), ())),
            preferred_element_type=jnp.float32,
        )
        term = picked * share[:, k : k + 1]
        total = term if total is None else total + term
    out_ref[...] = total.astype(jnp.bfloat16)


def expert_kernel(x_ref, gate_ref, up_ref, down_ref, out_ref, total):
    inputs = x_ref[...]
    gate_part = jnp.dot(inputs, gate_ref[...], preferred_element_type=jnp.float32)
    up_part = jnp.dot(inputs, up_ref[...], preferred_element_type=jnp.float32)
    hidden = (gate_part / (1.0 + jnp.exp(-gate_part)) * up_part).astype(jnp.bfloat16)
    part = jnp.dot(hidden, down_ref[...], preferred_element_type=jnp.float32)

    @pl.when(pl.program_id(0) == 0)
    def _():
        total[...] = part

    @pl.when(pl.program_id(0) != 0)
    def _():
        total[...] += part

    @pl.when(pl.program_id(0) == pl.num_programs(0) - 1)
    def _():
        out_ref[...] = total[...].astype(jnp.bfloat16)


def expert_apply(inputs, gate_w, up_w, down_w):
    rows, width = inputs.shape
    hidden = gate_w.shape[1]
    tile = math.gcd(hidden, 256)
    return pl.pallas_call(
        expert_kernel,
        out_shape=jax.ShapeDtypeStruct((rows, width), jnp.bfloat16),
        grid=(hidden // tile,),
        in_specs=[
            VMEM,
            pl.BlockSpec((width, tile), lambda i: (0, i)),
            pl.BlockSpec((width, tile), lambda i: (0, i)),
            pl.BlockSpec((tile, width), lambda i: (i, 0)),
        ],
        out_specs=VMEM,
        scratch_shapes=[pltpu.VMEM((rows, width), jnp.float32)],
        cost_estimate=pl.CostEstimate(
            flops=6 * rows * width * hidden,
            bytes_accessed=6 * width * hidden + 4 * rows * width,
            transcendentals=rows * hidden,
        ),
        name="experts",
    )(inputs, gate_w, up_w, down_w)


def body(
    queries,
    keys,
    values,
    query_gain,
    key_gain,
    out_proj,
    tokens_b,
    norm_gain,
    routes,
    group_prob,
    expert_logits,
    w_gate,
    w_up,
    w_down,
):
    device_count = lax.axis_size("ep") * lax.axis_size("tp")
    row_count, top_count = routes.shape
    model_width = tokens_b.shape[1]
    capacity = 2 * top_count * row_count // device_count
    head_dim = query_gain.shape[0]

    queries_in, block = attention_inputs(queries, keys, values, query_gain, key_gain)
    sender, slots = pl.pallas_call(
        functools.partial(dispatch_kernel, capacity, device_count),
        out_shape=(
            jax.ShapeDtypeStruct((device_count * capacity, model_width), jnp.bfloat16),
            jax.ShapeDtypeStruct((top_count, row_count), jnp.int32),
        ),
        in_specs=[VMEM] * 3,
        out_specs=(VMEM, VMEM),
        name="dispatch",
    )(routes.T, tokens_b, norm_gain.reshape(1, model_width))

    def exchange(rows):
        return lax.all_to_all(
            rows.reshape(device_count, capacity, model_width),
            ("ep", "tp"),
            split_axis=0,
            concat_axis=0,
            tiled=True,
        ).reshape(device_count * capacity, model_width)

    pieces, sender = gather_pieces(block, sender)
    arrived = exchange(sender)
    expert_out = expert_apply(arrived, w_gate[0], w_up[0], w_down[0])
    queries_in, expert_out = lax.optimization_barrier((queries_in, expert_out))
    returned = exchange(expert_out)
    attended = attend(queries_in, pieces, head_dim)
    mixed_a = project(attended, out_proj)
    mixed_b = pl.pallas_call(
        combine_kernel,
        out_shape=jax.ShapeDtypeStruct((row_count, model_width), jnp.bfloat16),
        in_specs=[VMEM] * 4,
        out_specs=VMEM,
        name="combine",
    )(slots, group_prob.reshape(row_count, 1), expert_logits, returned)
    return (mixed_a, mixed_b)


def solution(mesh):
    placed = (
        P("ep", "tp"),
        P("ep", "tp"),
        P("ep", "tp"),
        P(),
        P(),
        P(),
        P(("ep", "tp"), None),
        P(),
        P(("ep", "tp"), None),
        P(("ep", "tp")),
        P(("ep", "tp"), None),
        P(("ep", "tp"), None, None),
        P(("ep", "tp"), None, None),
        P(("ep", "tp"), None, None),
    )
    return jax.shard_map(
        body,
        mesh=mesh,
        in_specs=placed,
        out_specs=(P(("ep", "tp"), None), P(("ep", "tp"), None)),
        check_vma=False,
    )
```
